32 devices in a mesh: ra: 8 (over z, x), cb: 4 (over y, core).
Axes of the slice: x: 2, y: 2, z: 4, core: 2. Of those that a mesh axis runs over, the one named last changes fastest.
Arguments:
- tokens: bfloat16 [384, 4096], P(None, 'ra'), may hold values from -260 to 260
- up_weight: float32 [2, 4096, 16384], P(None, 'ra', 'cb'), may hold values from -0.125 to 0.125
- up_scale: float32 [2, 16384], P(None, 'cb'), may hold values from 0.5 to 2
- down_weight: float32 [2, 16384, 4096], P(None, 'cb', 'ra'), may hold values from -0.046875 to 0.046875
- down_scale: float32 [2, 4096], P(None, 'ra'), may hold values from 0.7 to 14
- pre_gain: float32 [2, 4096], P(None, 'ra'), may hold values from 0.1 to 1.9
- post_gain: float32 [2, 4096], P(None, 'ra'), may hold values from 0.1 to 1.9
Outputs:
- stream_out: bfloat16 [384, 4096], P(None, 'ra')
The draws below stay inside these ranges and needn't reach their ends.
All inputs are finite; a program needn't handle non-finite values.
Results may differ from the reference program's by a relative error of at most 0.023.
Values may be sent and summed in bfloat16 or wider, within the bound.
A program may use at most 128 MiB of HBM per device.

```python
import math
import jax
import jax.numpy as jnp
from jax import lax

D = 4096
FF = 16384
LAYERS = 2
TOKENS = 384
N_CB = 4


def draw_tokens(key, part):
    first = jax.random.fold_in(key, 11)
    second = jax.random.fold_in(key, 12)
    third = jax.random.fold_in(key, 13)
    column_scale = 10.0 ** (jnp.arange(D, dtype=jnp.float32) / D) * jax.random.uniform(second, (D,), jnp.float32, 0.7, 1.4)
    row_scale = 10.0 ** jax.random.uniform(third, (TOKENS, 1), jnp.float32)
    base = jnp.clip(jax.random.normal(first, (TOKENS, D), jnp.float32), -6.0, 6.0)
    return (0.3 * base * row_scale * column_scale[None, :]).astype(jnp.bfloat16)


def draw_down_scale(key, part):
    first = jax.random.fold_in(key, 21)
    rising = 10.0 ** (jnp.arange(D, dtype=jnp.float32) / D)
    rough = jnp.exp(jax.random.uniform(first, (LAYERS, D), jnp.float32, jnp.log(0.7), jnp.log(1.4)))
    return (rough * rising[None, :]).astype(jnp.float32)


def strengthened(entries, rng, source, target, parts, factor):
    def block_of(dim):
        return (jnp.arange(entries.shape[dim]) // (entries.shape[dim] // parts)).reshape((-1,) + (1,) * (entries.ndim - 1 - dim))

    one_side = jax.random.permutation(rng, parts)[block_of(target)]
    second = (block_of(target) + parts // 2) % parts
    return jnp.where((block_of(source) == one_side) | (block_of(source) == second), factor * entries, entries)


def block_scale(stream_key, dims, shards, smallest, largest):
    def one(dim, shards_of):
        draws = jax.random.uniform(jax.random.fold_in(jax.random.fold_in(stream_key, 6), dim), (shards_of,), jnp.float32, smallest / len(shards), largest / len(shards))
        return jnp.repeat(jnp.exp(draws), dims[dim] // shards_of).reshape((-1,) + (1,) * (len(dims) - dim - 1))

    factor_of = one(*shards[0])
    for cut in shards[1:]:
        factor_of = factor_of * one(*cut)
    return factor_of


def gaussian(key, dims, width, bound, pieces=(), held_as=jnp.bfloat16):
    loudness = block_scale(key, dims, pieces, -0.22, 0.18) if pieces else 1.0
    values = jax.random.normal(key, dims, jnp.float32) * width * loudness
    return jnp.minimum(jnp.maximum(values, -bound), bound).astype(held_as)


def heavy_noise(own_key, extent, deviation, limit, split, heavy, held_as=jnp.bfloat16):
    drawn = deviation * jax.random.normal(own_key, extent, jnp.float32)
    if split:
        drawn = drawn * block_scale(own_key, extent, split, -0.22, 0.18)
    return jnp.clip(strengthened(drawn, jax.random.fold_in(own_key, 3), *heavy), -limit, limit).astype(held_as)


def setup_inputs(seed: int = 0) -> dict:
    key_of = jax.random.split(jax.random.key(seed), 8)
    return {
        "tokens": draw_tokens(jax.random.fold_in(key_of[7], 71), 0),
        "up_weight": heavy_noise(key_of[1], (LAYERS, D, FF), D ** -0.5, 0.125, ((1, 8), (2, 4)), (1, 2, 8, 2.0), jnp.float32),
        "up_scale": jnp.clip(jnp.exp(math.log(2.0) - 1.3862944 * jax.random.uniform(key_of[2], (LAYERS, FF), jnp.float32) ** block_scale(key_of[2], (LAYERS, FF), ((1, 4),), -0.2, 0.2)), 0.5, 2.0),
        "down_weight": gaussian(key_of[3], (LAYERS, FF, D), FF ** -0.5, 0.046875, ((1, 4), (2, 8)), jnp.float32),
        "down_scale": draw_down_scale(jax.random.fold_in(key_of[7], 71), 0),
        "pre_gain": jnp.clip(1.0 + 0.18 * jax.random.normal(key_of[5], (LAYERS, D), jnp.float32), 0.1, 1.9),
        "post_gain": jnp.clip(1.0 + 0.18 * jax.random.normal(key_of[6], (LAYERS, D), jnp.float32), 0.1, 1.9),
    }


norm_eps = 1e-06
residual_keep = 0.5

def reference(tokens, up_weight, up_scale, down_weight, down_scale, pre_gain, post_gain):
    stream = tokens
    for sublayer in range(LAYERS):
        values = stream.astype(jnp.float32)
        scaled = (values * pre_gain[sublayer][None, :]).astype(jnp.bfloat16)
        whole_up = jnp.dot(scaled, up_weight[sublayer].astype(jnp.bfloat16), preferred_element_type=jnp.float32)
        whole_up = whole_up * up_scale[sublayer][None, :]
        hidden = jnp.square(jax.nn.relu(whole_up)).astype(jnp.bfloat16)
        block_hidden = hidden.reshape(TOKENS, N_CB, FF // N_CB).astype(jnp.float32)
        block_down = down_weight[sublayer].astype(jnp.bfloat16).reshape(N_CB, FF // N_CB, D).astype(jnp.float32)
        partials = jnp.einsum('mbf,bfd->bmd', block_hidden, block_down).astype(jnp.bfloat16)
        partials = lax.optimization_barrier(partials).astype(jnp.float32)
        branch_in = lax.optimization_barrier(jnp.sum(partials, axis=0)) * down_scale[sublayer][None, :]
        inv_post = lax.rsqrt(lax.optimization_barrier(jnp.mean(branch_in * branch_in, axis=1, keepdims=True)) + norm_eps)
        branch = branch_in * inv_post * post_gain[sublayer][None, :]
        stream = (residual_keep * values + branch).astype(jnp.bfloat16)
    return stream
```

```python
import functools

import jax
import jax.numpy as jnp
from jax import lax
from jax.experimental import pallas as pl
from jax.experimental.pallas import tpu as pltpu
from jax.sharding import PartitionSpec as P

norm_eps = 1e-06
residual_keep = 0.5
MESH = pl.DeviceIdType.MESH
FLOWS = 4
LANES = 128
BF16_ROWS = 16


def plain(tokens, up_weight, up_scale, down_weight, down_scale, pre_gain, post_gain):
    values = tokens.astype(jnp.float32)
    model_width = tokens.shape[1] * lax.axis_size("ra")
    stream = tokens
    for sublayer in range(up_weight.shape[0]):
        scaled = (values * pre_gain[sublayer][None, :]).astype(jnp.bfloat16)
        up_matrix = up_weight[sublayer].astype(jnp.bfloat16)
        down_matrix = down_weight[sublayer].astype(jnp.bfloat16)
        partial_up = jnp.dot(scaled, up_matrix, preferred_element_type=jnp.float32)
        whole_up = lax.psum(partial_up.astype(jnp.bfloat16), "ra").astype(jnp.float32)
        hidden = jnp.square(jax.nn.relu(whole_up * up_scale[sublayer][None, :])).astype(
            jnp.bfloat16
        )
        partial_down = jnp.dot(hidden, down_matrix, preferred_element_type=jnp.float32)
        summed = lax.psum(partial_down.astype(jnp.bfloat16), "cb").astype(jnp.float32)
        branch_in = summed * down_scale[sublayer][None, :]
        post_squares = lax.psum(jnp.sum(branch_in * branch_in, axis=1), "ra")
        inv_post = lax.rsqrt(post_squares / model_width + norm_eps)[:, None]
        branch = branch_in * inv_post * post_gain[sublayer][None, :]
        stream = (residual_keep * values + branch).astype(jnp.bfloat16)
        values = stream.astype(jnp.float32)
    return stream


def kernel(
    n, m, layers,
    tok, up, us, dn, ds, pg, qg,
    out,
    st_up, st_dn, wu, wd, xs, own, sendb, recvb, hid, accd, cbb, bbuf, ssq, ssall,
    w_sem, rs_s, rs_r, ag_s, ag_r, cb_s, cb_r, ss_s, ss_r,
):
    f32, bf16 = jnp.float32, jnp.bfloat16
    ra, cb = lax.axis_index("ra"), lax.axis_index("cb")
    rows, dl = tok.shape[1], tok.shape[2]
    fq = wu.shape[2]
    tokens = n * rows

    def wrap(i):
        return lax.rem(i + 2 * n, n)

    half, odd = lax.div(ra, 2), lax.rem(ra, 2)
    p = half + odd * (n - 1 - 2 * half)

    def ra_of(q):
        hi = lax.div(q, n // 2)
        return 2 * q * (1 - hi) + hi * (2 * (n - 1 - q) + 1)

    right, left = ra_of(wrap(p + 1)), ra_of(wrap(p - 1))
    order = [0, FLOWS // 2] + [1, FLOWS // 2 + 1]
    sign = [1 if f < FLOWS // 2 else -1 for f in range(FLOWS)]
    target = [right if f < FLOWS // 2 else left for f in range(FLOWS)]

    def up_copy(l, f):
        return pltpu.make_async_copy(
            up.at[l, :, pl.ds(f * fq, fq)], st_up.at[f], w_sem.at[0, f]
        )

    def dn_copy(l, f):
        return pltpu.make_async_copy(
            dn.at[l, pl.ds(f * fq, fq), :], st_dn.at[f], w_sem.at[1, f]
        )

    def convert(src, dst, f, block):
        def body(i, _):
            r = pl.ds(pl.multiple_of(i * block, block), block)
            dst[f, r, :] = src[f, r, :].astype(bf16)
            return 0

        lax.fori_loop(0, src.shape[1] // block, body, 0)

    def convert_up(l):
        for f in order:
            up_copy(l, f).wait()
            convert(st_up, wu, f, min(64, dl))
        if l + 1 < layers:
            for f in order:
                up_copy(l + 1, f).start()

    def convert_dn(l):
        for f in order:
            dn_copy(l, f).wait()
            convert(st_dn, wd, f, min(128, fq))
        if l + 1 < layers:
            for f in order:
                dn_copy(l + 1, f).start()

    def rs_copy(l, f, s):
        return pltpu.make_async_remote_copy(
            src_ref=sendb.at[f, s], dst_ref=recvb.at[l, f, s],
            send_sem=rs_s.at[l, f, s], recv_sem=rs_r.at[l, f, s],
            device_id={"ra": target[f]}, device_id_type=MESH,
        )

    def ag_copy(l, f, s):
        c = wrap(p - sign[f] * (s - 1))
        return pltpu.make_async_remote_copy(
            src_ref=hid.at[l, c, f], dst_ref=hid.at[l, c, f],
            send_sem=ag_s.at[l, f, s - 1], recv_sem=ag_r.at[l, f, s - 1],
            device_id={"ra": target[f]}, device_id_type=MESH,
        )

    def ag_arrival(l, f, s):
        c = wrap(p - sign[f] * s)
        return pltpu.make_async_remote_copy(
            src_ref=hid.at[l, c, f], dst_ref=hid.at[l, c, f],
            send_sem=ag_s.at[l, f, s - 1], recv_sem=ag_r.at[l, f, s - 1],
            device_id={"ra": target[f]}, device_id_type=MESH,
        )

    def cb_copy(l, k, c, who):
        return pltpu.make_async_remote_copy(
            src_ref=cbb.at[l, who, c], dst_ref=cbb.at[l, who, c],
            send_sem=cb_s.at[l, k - 1, c], recv_sem=cb_r.at[l, k - 1, c],
            device_id={"cb": lax.rem(cb + k, m)}, device_id_type=MESH,
        )

    def ss_copy(l, k, who):
        return pltpu.make_async_remote_copy(
            src_ref=ssall.at[l, who], dst_ref=ssall.at[l, who],
            send_sem=ss_s.at[l, k - 1], recv_sem=ss_r.at[l, k - 1],
            device_id={"ra": lax.rem(ra + k, n)}, device_id_type=MESH,
        )

    def dot(a, b):
        return jnp.dot(a, b, preferred_element_type=f32)

    for f in order:
        up_copy(0, f).start()
    for f in order:
        dn_copy(0, f).start()

    barrier = pltpu.get_barrier_semaphore()
    for k in range(1, n):
        pl.semaphore_signal(
            barrier, inc=1, device_id={"ra": lax.rem(ra + k, n)}, device_id_type=MESH
        )
    for k in range(1, m):
        pl.semaphore_signal(
            barrier, inc=1, device_id={"cb": lax.rem(cb + k, m)}, device_id_type=MESH
        )

    def scale_in(c, _):
        xs[c] = (tok[c].astype(f32) * pg[0:1, :]).astype(bf16)
        return 0

    lax.fori_loop(0, n, scale_in, 0)
    pl.semaphore_wait(barrier, n + m - 2)

    for l in range(layers):
        if l == 0:
            for f in order:
                up_copy(l, f).wait()
                convert(st_up, wu, f, min(64, dl))
                sendb[f, 0] = dot(xs[wrap(p - sign[f])], wu[f]).astype(bf16)
                rs_copy(l, f, 0).start()
            for f in order:
                if layers > 1:
                    up_copy(l + 1, f).start()
        else:
            for f in order:
                sendb[f, 0] = dot(xs[wrap(p - sign[f])], wu[f]).astype(bf16)
                rs_copy(l, f, 0).start()
        convert_dn(l)

        def rs_step(s, _):
            for f in order:
                own[f] = dot(xs[wrap(p - sign[f] * (2 + s))], wu[f])
            for f in order:
                rs_copy(l, f, s).wait_recv()
                sendb[f, s + 1] = (recvb[l, f, s].astype(f32) + own[f]).astype(bf16)
                rs_copy(l, f, s + 1).start()
            return 0

        lax.fori_loop(0, n - 2, rs_step, 0)
        for f in order:
            own[f] = dot(xs[p], wu[f])
        for f in order:
            rs_copy(l, f, n - 2).wait_recv()
            v = recvb[l, f, n - 2].astype(f32) + own[f]
            v = jnp.maximum(v * us[l : l + 1, f * fq : (f + 1) * fq], 0.0)
            hid[l, p, f] = (v * v).astype(bf16)
            ag_copy(l, f, 1).start()

        def finish(c):
            cbb[l, cb, c] = accd[c].astype(bf16)
            for k in range(1, m):
                cb_copy(l, k, c, cb).start()

        def zero(c, _):
            accd[c] = jnp.zeros_like(accd[c])
            return 0

        lax.fori_loop(0, n, zero, 0)
        a = dot(hid[l, p, 0], wd[0])
        for f in range(1, FLOWS):
            a = a + dot(hid[l, p, f], wd[f])
        accd[p] = a
        finish(p)
        if l + 1 < layers:
            for f in order:
                up_copy(l + 1, f).wait()
                convert(st_up, wu, f, min(64, dl))
            if l + 2 < layers:
                for f in order:
                    up_copy(l + 2, f).start()

        def ag_step(s, _):
            for f in order:
                ag_arrival(l, f, s).wait_recv()

                @pl.when(s < n - 1)
                def _():
                    ag_copy(l, f, s + 1).start()

            cr, cl = wrap(p - s), wrap(p + s)
            h = FLOWS // 2
            accd[cr] += sum(dot(hid[l, cr, f], wd[f]) for f in range(h))
            accd[cl] += sum(dot(hid[l, cl, f], wd[f]) for f in range(h, FLOWS))

            @pl.when(s >= n // 2)
            def _():
                finish(cr)

            @pl.when(s > n // 2)
            def _():
                finish(cl)

            return 0

        lax.fori_loop(1, n, ag_step, 0)

        def gather_in(c):
            for k in range(1, m):
                cb_copy(l, k, c, lax.rem(cb + m - k, m)).wait_recv()
            b = cbb[l, 0, c].astype(f32)
            for k in range(1, m):
                b = b + cbb[l, k, c].astype(f32)
            b = b * ds[l : l + 1, :]
            bbuf[c] = b
            b = b * b
            t = b[:, :LANES]
            for j in range(1, dl // LANES):
                t = t + b[:, j * LANES : (j + 1) * LANES]
            ssq[c] = t

        def gather_pair(s, _):
            gather_in(wrap(p - s))
            gather_in(wrap(p + s))
            return 0

        gather_in(p)
        gather_in(wrap(p + n // 2))
        lax.fori_loop(n // 2 + 1, n, gather_pair, 0)

        t = jnp.transpose(ssq[...].reshape(tokens, LANES))
        t = jnp.sum(t, axis=0, keepdims=True)
        ssall[l, ra] = jnp.broadcast_to(t, (8, tokens))
        for k in range(1, n):
            ss_copy(l, k, ra).start()
        for k in range(1, n):
            ss_copy(l, k, lax.rem(ra + n - k, n)).wait_recv()
        t = ssall[l, 0]
        for k in range(1, n):
            t = t + ssall[l, k]
        t = lax.rsqrt(t / (dl * n) + norm_eps)
        t = jnp.broadcast_to(t[0:1, :], (LANES, tokens))
        ssq[...] = jnp.transpose(t).reshape(n, rows, LANES)

        before = tok if l == 0 else out

        def renew(c, _):
            inv = ssq[c]
            for j in range(dl // LANES):
                col = slice(j * LANES, (j + 1) * LANES)
                branch = bbuf[c, :, col] * inv * qg[l : l + 1, col]
                new = (residual_keep * before[c, :, col].astype(f32) + branch).astype(bf16)
                out[c, :, col] = new
                if l + 1 < layers:
                    xs[c, :, col] = (new.astype(f32) * pg[l + 1 : l + 2, col]).astype(bf16)
            return 0

        lax.fori_loop(0, n, renew, 0)

        def drain(s, _):
            for f in order:
                rs_copy(l, f, s).wait_send()
                ag_copy(l, f, s + 1).wait_send()
            return 0

        lax.fori_loop(0, n - 1, drain, 0)

        def drain_cb(c, _):
            for k in range(1, m):
                cb_copy(l, k, c, cb).wait_send()
            return 0

        lax.fori_loop(0, n, drain_cb, 0)
        for k in range(1, n):
            ss_copy(l, k, ra).wait_send()


def local(n, m, tokens, up_weight, up_scale, down_weight, down_scale, pre_gain, post_gain):
    t, dl = tokens.shape
    layers, _, fl = up_weight.shape
    fits = (
        n % 2 == 0 and n >= 4 and m >= 2 and t % (n * BF16_ROWS) == 0 and t % LANES == 0
        and fl % (FLOWS * LANES) == 0 and dl % LANES == 0
    )
    if not fits:
        return plain(
            tokens, up_weight, up_scale, down_weight, down_scale, pre_gain, post_gain
        )
    rows, fq = t // n, fl // FLOWS
    f32, bf16 = jnp.float32, jnp.bfloat16
    vmem = pl.BlockSpec(memory_space=pltpu.VMEM)
    hbm = pl.BlockSpec(memory_space=pl.ANY)
    dma = pltpu.SemaphoreType.DMA
    out = pl.pallas_call(
        functools.partial(kernel, n, m, layers),
        out_shape=jax.ShapeDtypeStruct((n, rows, dl), bf16),
        in_specs=[vmem, hbm, vmem, hbm, vmem, vmem, vmem],
        out_specs=vmem,
        scratch_shapes=[
            pltpu.VMEM((FLOWS, dl, fq), f32),
            pltpu.VMEM((FLOWS, fq, dl), f32),
            pltpu.VMEM((FLOWS, dl, fq), bf16),
            pltpu.VMEM((FLOWS, fq, dl), bf16),
            pltpu.VMEM((n, rows, dl), bf16),
            pltpu.VMEM((FLOWS, rows, fq), f32),
            pltpu.VMEM((FLOWS, n - 1, rows, fq), bf16),
            pltpu.VMEM((layers, FLOWS, n - 1, rows, fq), bf16),
            pltpu.VMEM((layers, n, FLOWS, rows, fq), bf16),
            pltpu.VMEM((n, rows, dl), f32),
            pltpu.VMEM((layers, m, n, rows, dl), bf16),
            pltpu.VMEM((n, rows, dl), f32),
            pltpu.VMEM((n, rows, LANES), f32),
            pltpu.VMEM((layers, n, 8, t), f32),
            dma((2, FLOWS)),
            dma((layers, FLOWS, n - 1)),
            dma((layers, FLOWS, n - 1)),
            dma((layers, FLOWS, n - 1)),
            dma((layers, FLOWS, n - 1)),
            dma((layers, m - 1, n)),
            dma((layers, m - 1, n)),
            dma((layers, n - 1)),
            dma((layers, n - 1)),
        ],
        compiler_params=pltpu.CompilerParams(
            collective_id=0, has_side_effects=True, vmem_limit_bytes=60 * 1024 * 1024
        ),
    )(
        tokens.reshape(n, rows, dl), up_weight, up_scale, down_weight, down_scale,
        pre_gain, post_gain,
    )
    return out.reshape(t, dl)


def solution(mesh):
    return jax.shard_map(
        functools.partial(local, mesh.shape["ra"], mesh.shape["cb"]),
        mesh=mesh,
        in_specs=(
            P(None, "ra"),
            P(None, "ra", "cb"),
            P(None, "cb"),
            P(None, "cb", "ra"),
            P(None, "ra"),
            P(None, "ra"),
            P(None, "ra"),
        ),
        out_specs=P(None, "ra"),
        check_vma=False,
    )
```

```python
import functools

import jax
import jax.numpy as jnp
from jax import lax
from jax.experimental import pallas as pl
from jax.experimental.pallas import tpu as pltpu
from jax.sharding import PartitionSpec as P

norm_eps = 1e-06
residual_keep = 0.5
MESH = pl.DeviceIdType.MESH
FLOWS = 8
LANES = 128
BF16_ROWS = 16


def plain(tokens, up_weight, up_scale, down_weight, down_scale, pre_gain, post_gain):
    values = tokens.astype(jnp.float32)
    model_width = tokens.shape[1] * lax.axis_size("ra")
    stream = tokens
    for sublayer in range(up_weight.shape[0]):
        scaled = (values * pre_gain[sublayer][None, :]).astype(jnp.bfloat16)
        up_matrix = up_weight[sublayer].astype(jnp.bfloat16)
        down_matrix = down_weight[sublayer].astype(jnp.bfloat16)
        partial_up = jnp.dot(scaled, up_matrix, preferred_element_type=jnp.float32)
        whole_up = lax.psum(partial_up.astype(jnp.bfloat16), "ra").astype(jnp.float32)
        hidden = jnp.square(jax.nn.relu(whole_up * up_scale[sublayer][None, :])).astype(
            jnp.bfloat16
        )
        partial_down = jnp.dot(hidden, down_matrix, preferred_element_type=jnp.float32)
        summed = lax.psum(partial_down.astype(jnp.bfloat16), "cb").astype(jnp.float32)
        branch_in = summed * down_scale[sublayer][None, :]
        post_squares = lax.psum(jnp.sum(branch_in * branch_in, axis=1), "ra")
        inv_post = lax.rsqrt(post_squares / model_width + norm_eps)[:, None]
        branch = branch_in * inv_post * post_gain[sublayer][None, :]
        stream = (residual_keep * values + branch).astype(jnp.bfloat16)
        values = stream.astype(jnp.float32)
    return stream


def kernel(
    n, m, layers,
    tok, up, us, dn, ds, pg, qg,
    out,
    st_up, st_dn, wu, wd, xs, own, sendb, recvb, hid, accd, cbb, bbuf, ssq, ssall,
    w_sem, rs_s, rs_r, ag_s, ag_r, cb_s, cb_r, ss_s, ss_r,
):
    f32, bf16 = jnp.float32, jnp.bfloat16
    ra, cb = lax.axis_index("ra"), lax.axis_index("cb")
    rows, dl = tok.shape[1], tok.shape[2]
    fq = wu.shape[2]
    tokens = n * rows

    def wrap(i):
        return lax.rem(i + 2 * n, n)

    half, odd = lax.div(ra, 2), lax.rem(ra, 2)
    p = half + odd * (n - 1 - 2 * half)

    def ra_of(q):
        hi = lax.div(q, n // 2)
        return 2 * q * (1 - hi) + hi * (2 * (n - 1 - q) + 1)

    right, left = ra_of(wrap(p + 1)), ra_of(wrap(p - 1))
    order = [i + j for i in range(FLOWS // 2) for j in (0, FLOWS // 2)]
    sign = [1 if f < FLOWS // 2 else -1 for f in range(FLOWS)]
    target = [right if f < FLOWS // 2 else left for f in range(FLOWS)]

    def up_copy(l, f):
        return pltpu.make_async_copy(
            up.at[l, :, pl.ds(f * fq, fq)], st_up.at[f], w_sem.at[0, f]
        )

    def dn_copy(l, f):
        return pltpu.make_async_copy(
            dn.at[l, pl.ds(f * fq, fq), :], st_dn.at[f], w_sem.at[1, f]
        )

    def convert(src, dst, f, block):
        def body(i, _):
            r = pl.ds(pl.multiple_of(i * block, block), block)
            dst[f, r, :] = src[f, r, :].astype(bf16)
            return 0

        lax.fori_loop(0, src.shape[1] // block, body, 0)

    def convert_up(l):
        for f in order:
            up_copy(l, f).wait()
            convert(st_up, wu, f, min(64, dl))
        if l + 1 < layers:
            for f in order:
                up_copy(l + 1, f).start()

    def convert_dn(l):
        for f in order:
            dn_copy(l, f).wait()
            convert(st_dn, wd, f, min(128, fq))
        if l + 1 < layers:
            for f in order:
                dn_copy(l + 1, f).start()

    def rs_copy(l, f, s):
        return pltpu.make_async_remote_copy(
            src_ref=sendb.at[f, s], dst_ref=recvb.at[l, f, s],
            send_sem=rs_s.at[l, f, s], recv_sem=rs_r.at[l, f, s],
            device_id={"ra": target[f]}, device_id_type=MESH,
        )

    def ag_copy(l, f, s):
        c = wrap(p - sign[f] * (s - 1))
        return pltpu.make_async_remote_copy(
            src_ref=hid.at[l, c, f], dst_ref=hid.at[l, c, f],
            send_sem=ag_s.at[l, f, s - 1], recv_sem=ag_r.at[l, f, s - 1],
            device_id={"ra": target[f]}, device_id_type=MESH,
        )

    def ag_arrival(l, f, s):
        c = wrap(p - sign[f] * s)
        return pltpu.make_async_remote_copy(
            src_ref=hid.at[l, c, f], dst_ref=hid.at[l, c, f],
            send_sem=ag_s.at[l, f, s - 1], recv_sem=ag_r.at[l, f, s - 1],
            device_id={"ra": target[f]}, device_id_type=MESH,
        )

    def cb_copy(l, k, c, who):
        return pltpu.make_async_remote_copy(
            src_ref=cbb.at[l, who, c], dst_ref=cbb.at[l, who, c],
            send_sem=cb_s.at[l, k - 1, c], recv_sem=cb_r.at[l, k - 1, c],
            device_id={"cb": lax.rem(cb + k, m)}, device_id_type=MESH,
        )

    def ss_copy(l, k, who):
        return pltpu.make_async_remote_copy(
            src_ref=ssall.at[l, who], dst_ref=ssall.at[l, who],
            send_sem=ss_s.at[l, k - 1], recv_sem=ss_r.at[l, k - 1],
            device_id={"ra": lax.rem(ra + k, n)}, device_id_type=MESH,
        )

    def dot(a, b):
        return jnp.dot(a, b, preferred_element_type=f32)

    for f in order:
        up_copy(0, f).start()
    for f in order:
        dn_copy(0, f).start()

    barrier = pltpu.get_barrier_semaphore()
    for k in range(1, n):
        pl.semaphore_signal(
            barrier, inc=1, device_id={"ra": lax.rem(ra + k, n)}, device_id_type=MESH
        )
    for k in range(1, m):
        pl.semaphore_signal(
            barrier, inc=1, device_id={"cb": lax.rem(cb + k, m)}, device_id_type=MESH
        )

    def scale_in(c, _):
        xs[c] = (tok[c].astype(f32) * pg[0:1, :]).astype(bf16)
        return 0

    lax.fori_loop(0, n, scale_in, 0)
    pl.semaphore_wait(barrier, n + m - 2)

    for l in range(layers):
        if l == 0:
            for f in order:
                up_copy(l, f).wait()
                convert(st_up, wu, f, min(64, dl))
                sendb[f, 0] = dot(xs[wrap(p - sign[f])], wu[f]).astype(bf16)
                rs_copy(l, f, 0).start()
            for f in order:
                if layers > 1:
                    up_copy(l + 1, f).start()
        else:
            for f in order:
                sendb[f, 0] = dot(xs[wrap(p - sign[f])], wu[f]).astype(bf16)
                rs_copy(l, f, 0).start()
        convert_dn(l)

        def rs_step(s, _):
            for f in order:
                own[f] = dot(xs[wrap(p - sign[f] * (2 + s))], wu[f])
            for f in order:
                rs_copy(l, f, s).wait_recv()
                sendb[f, s + 1] = (recvb[l, f, s].astype(f32) + own[f]).astype(bf16)
                rs_copy(l, f, s + 1).start()
            return 0

        lax.fori_loop(0, n - 2, rs_step, 0)
        for f in order:
            own[f] = dot(xs[p], wu[f])
        for f in order:
            rs_copy(l, f, n - 2).wait_recv()
            v = recvb[l, f, n - 2].astype(f32) + own[f]
            v = jnp.maximum(v * us[l : l + 1, f * fq : (f + 1) * fq], 0.0)
            hid[l, p, f] = (v * v).astype(bf16)
            ag_copy(l, f, 1).start()

        def finish(c):
            cbb[l, cb, c] = accd[c].astype(bf16)
            for k in range(1, m):
                cb_copy(l, k, c, cb).start()

        def zero(c, _):
            accd[c] = jnp.zeros_like(accd[c])
            return 0

        lax.fori_loop(0, n, zero, 0)
        a = dot(hid[l, p, 0], wd[0])
        for f in range(1, FLOWS):
            a = a + dot(hid[l, p, f], wd[f])
        accd[p] = a
        finish(p)
        if l + 1 < layers:
            for f in order:
                up_copy(l + 1, f).wait()
                convert(st_up, wu, f, min(64, dl))
            if l + 2 < layers:
                for f in order:
                    up_copy(l + 2, f).start()

        def ag_step(s, _):
            for f in order:
                ag_arrival(l, f, s).wait_recv()

                @pl.when(s < n - 1)
                def _():
                    ag_copy(l, f, s + 1).start()

            cr, cl = wrap(p - s), wrap(p + s)
            h = FLOWS // 2
            accd[cr] += sum(dot(hid[l, cr, f], wd[f]) for f in range(h))
            accd[cl] += sum(dot(hid[l, cl, f], wd[f]) for f in range(h, FLOWS))

            @pl.when(s >= n // 2)
            def _():
                finish(cr)

            @pl.when(s > n // 2)
            def _():
                finish(cl)

            return 0

        lax.fori_loop(1, n, ag_step, 0)

        def gather_in(c):
            for k in range(1, m):
                cb_copy(l, k, c, lax.rem(cb + m - k, m)).wait_recv()
            b = cbb[l, 0, c].astype(f32)
            for k in range(1, m):
                b = b + cbb[l, k, c].astype(f32)
            b = b * ds[l : l + 1, :]
            bbuf[c] = b
            b = b * b
            t = b[:, :LANES]
            for j in range(1, dl // LANES):
                t = t + b[:, j * LANES : (j + 1) * LANES]
            ssq[c] = t

        def gather_pair(s, _):
            gather_in(wrap(p - s))
            gather_in(wrap(p + s))
            return 0

        gather_in(p)
        gather_in(wrap(p + n // 2))
        lax.fori_loop(n // 2 + 1, n, gather_pair, 0)

        t = jnp.transpose(ssq[...].reshape(tokens, LANES))
        t = jnp.sum(t, axis=0, keepdims=True)
        ssall[l, ra] = jnp.broadcast_to(t, (8, tokens))
        for k in range(1, n):
            ss_copy(l, k, ra).start()
        for k in range(1, n):
            ss_copy(l, k, lax.rem(ra + n - k, n)).wait_recv()
        t = ssall[l, 0]
        for k in range(1, n):
            t = t + ssall[l, k]
        t = lax.rsqrt(t / (dl * n) + norm_eps)
        t = jnp.broadcast_to(t[0:1, :], (LANES, tokens))
        ssq[...] = jnp.transpose(t).reshape(n, rows, LANES)

        before = tok if l == 0 else out

        def renew(c, _):
            inv = ssq[c]
            for j in range(dl // LANES):
                col = slice(j * LANES, (j + 1) * LANES)
                branch = bbuf[c, :, col] * inv * qg[l : l + 1, col]
                new = (residual_keep * before[c, :, col].astype(f32) + branch).astype(bf16)
                out[c, :, col] = new
                if l + 1 < layers:
                    xs[c, :, col] = (new.astype(f32) * pg[l + 1 : l + 2, col]).astype(bf16)
            return 0

        lax.fori_loop(0, n, renew, 0)

        def drain(s, _):
            for f in order:
                rs_copy(l, f, s).wait_send()
                ag_copy(l, f, s + 1).wait_send()
            return 0

        lax.fori_loop(0, n - 1, drain, 0)

        def drain_cb(c, _):
            for k in range(1, m):
                cb_copy(l, k, c, cb).wait_send()
            return 0

        lax.fori_loop(0, n, drain_cb, 0)
        for k in range(1, n):
            ss_copy(l, k, ra).wait_send()


def local(n, m, tokens, up_weight, up_scale, down_weight, down_scale, pre_gain, post_gain):
    t, dl = tokens.shape
    layers, _, fl = up_weight.shape
    fits = (
        n % 2 == 0 and n >= 4 and m >= 2 and t % (n * BF16_ROWS) == 0 and t % LANES == 0
        and fl % (FLOWS * LANES) == 0 and dl % LANES == 0
    )
    if not fits:
        return plain(
            tokens, up_weight, up_scale, down_weight, down_scale, pre_gain, post_gain
        )
    rows, fq = t // n, fl // FLOWS
    f32, bf16 = jnp.float32, jnp.bfloat16
    vmem = pl.BlockSpec(memory_space=pltpu.VMEM)
    hbm = pl.BlockSpec(memory_space=pl.ANY)
    dma = pltpu.SemaphoreType.DMA
    out = pl.pallas_call(
        functools.partial(kernel, n, m, layers),
        out_shape=jax.ShapeDtypeStruct((n, rows, dl), bf16),
        in_specs=[vmem, hbm, vmem, hbm, vmem, vmem, vmem],
        out_specs=vmem,
        scratch_shapes=[
            pltpu.VMEM((FLOWS, dl, fq), f32),
            pltpu.VMEM((FLOWS, fq, dl), f32),
            pltpu.VMEM((FLOWS, dl, fq), bf16),
            pltpu.VMEM((FLOWS, fq, dl), bf16),
            pltpu.VMEM((n, rows, dl), bf16),
            pltpu.VMEM((FLOWS, rows, fq), f32),
            pltpu.VMEM((FLOWS, n - 1, rows, fq), bf16),
            pltpu.VMEM((layers, FLOWS, n - 1, rows, fq), bf16),
            pltpu.VMEM((layers, n, FLOWS, rows, fq), bf16),
            pltpu.VMEM((n, rows, dl), f32),
            pltpu.VMEM((layers, m, n, rows, dl), bf16),
            pltpu.VMEM((n, rows, dl), f32),
            pltpu.VMEM((n, rows, LANES), f32),
            pltpu.VMEM((layers, n, 8, t), f32),
            dma((2, FLOWS)),
            dma((layers, FLOWS, n - 1)),
            dma((layers, FLOWS, n - 1)),
            dma((layers, FLOWS, n - 1)),
            dma((layers, FLOWS, n - 1)),
            dma((layers, m - 1, n)),
            dma((layers, m - 1, n)),
            dma((layers, n - 1)),
            dma((layers, n - 1)),
        ],
        compiler_params=pltpu.CompilerParams(
            collective_id=0, has_side_effects=True, vmem_limit_bytes=60 * 1024 * 1024
        ),
    )(
        tokens.reshape(n, rows, dl), up_weight, up_scale, down_weight, down_scale,
        pre_gain, post_gain,
    )
    return out.reshape(t, dl)


def solution(mesh):
    return jax.shard_map(
        functools.partial(local, mesh.shape["ra"], mesh.shape["cb"]),
        mesh=mesh,
        in_specs=(
            P(None, "ra"),
            P(None, "ra", "cb"),
            P(None, "cb"),
            P(None, "cb", "ra"),
            P(None, "ra"),
            P(None, "ra"),
            P(None, "ra"),
        ),
        out_specs=P(None, "ra"),
        check_vma=False,
    )
```
